32 devices in a mesh: sp: 16 (over z, y, x), tp: 2 (over core).
Axes of the slice: x: 2, y: 2, z: 4, core: 2. Of those that a mesh axis runs over, the one named last changes fastest.
Arguments:
- block_source: bfloat16 [2048, 2048], P('sp'), may hold values from -28 to 28
- address_weights: bfloat16 [1024, 2048], P('tp'), may hold values from -0.125 to 0.125
- causal_filter_taps: float32 [4, 1024], P(None, 'tp'), may hold values from -3 to 3
- payload_vectors: bfloat16 [2048, 2048], P('sp', 'tp'), may hold values from -0.25 to 0.25
- probe_vectors: bfloat16 [2048, 1024], P('sp', 'tp'), may hold values from -0.5 to 0.5
- interval_preimage: float32 [2048, 32], P('sp', 'tp'), may hold values from -3.5 to 4
- channel_damping_exponent: float32 [32], P('tp'), may hold values from -14 to -3
- added_damping_jumps: float32 [2048, 32], P('sp', 'tp'), may hold values from -1 to 0
- sigmoid_argument: bfloat16 [2048, 2048], P('sp', 'tp'), may hold values from -6 to 6
- adjoint_of_result: bfloat16 [2048, 2048], P('sp', 'tp'), may hold values from -6 to 6
Outputs:
- key_weight_grad: float32 [1024, 2048], P('tp', 'sp')
- row_squares: float32 [1024], P('tp')
- input_grad: bfloat16 [2048, 2048], P('tp', 'sp')
- value_grad: bfloat16 [2048, 2048], P('sp', 'tp')
- query_grad: bfloat16 [2048, 1024], P('sp', 'tp')
- decay_grad: float32 [2048, 32], P('sp', 'tp')
- gate_grad: bfloat16 [2048, 2048], P('sp', 'tp')
The draws below stay inside these ranges and needn't reach their ends.
All inputs are finite; a program needn't handle non-finite values.
Results may differ from the reference program's by a relative error of at most 0.015.
Values may be sent and summed in bfloat16 or wider, within the bound.
A program may use at most 64 MiB of HBM per device.

```python
import math
import jax
import jax.numpy as jnp
from jax import lax

D = 2048
HEADS = 32
HEAD_DIM = 64
GROUPS = 8
STATE = 128
KCONV = 4
BLOCK = 128
TOK_DEV = 128
TOKENS = 2048
INNER = 2048
KEY_WIDTH = 1024
N_TP = 2


def draw_block_source(key, part):
    base_key, scale_key = jax.random.split(jax.random.fold_in(key, 101), 2)
    column = 3.0 ** (jnp.arange(D, dtype=jnp.float32) / D)
    column = column * jnp.exp(jax.random.uniform(scale_key, (D,), jnp.float32, -0.6, 0.6))
    noise = jnp.clip(jax.random.normal(base_key, (TOKENS, D), jnp.float32), -4.0, 4.0)
    return (noise * column[None]).astype(jnp.bfloat16)


def draw_interval_preimage(key, part):
    level_key, noise_key = jax.random.split(jax.random.fold_in(key, 202), 2)
    block_total = TOKENS // TOK_DEV
    levels = jax.random.uniform(level_key, (block_total, 1), jnp.float32, -1.0, 1.5)
    levels = jnp.repeat(levels, TOK_DEV, axis=0)
    noise = 0.7 * jnp.clip(jax.random.normal(noise_key, (TOKENS, HEADS), jnp.float32), -3.5, 3.5)
    return levels + noise


def draw_channel_damping_exponent(key, part):
    pick_key, slow_key, fast_key = jax.random.split(jax.random.fold_in(key, 303), 3)
    fast_share = 0.5
    slow_low = math.log(0.3 / TOKENS)
    slow_high = math.log(1.0 / 64.0)
    is_fast = jax.random.uniform(pick_key, (HEADS,), jnp.float32) < fast_share
    slow_rate = jnp.exp(jax.random.uniform(slow_key, (HEADS,), jnp.float32, slow_low, slow_high))
    fast_rate = jnp.exp(jax.random.uniform(fast_key, (HEADS,), jnp.float32, math.log(0.01), math.log(0.04)))
    return jnp.log(jnp.where(is_fast, fast_rate, slow_rate))


def draw_added_damping_jumps(key, part):
    spot_key, size_key = jax.random.split(jax.random.fold_in(key, 404), 2)
    spots = jax.random.randint(spot_key, (2, HEADS), 0, TOKENS)
    amounts = jax.random.uniform(size_key, (2, HEADS), jnp.float32, -0.5, -0.22)
    positions = jnp.arange(TOKENS, dtype=jnp.int32)[:, None]
    first = jnp.where(positions == spots[0][None], amounts[0][None], 0.0)
    second = jnp.where(positions == spots[1][None], amounts[1][None], 0.0)
    return (first + second).astype(jnp.float32)


def level_of(rng, dims, pieces, least, top_value):
    level, own = 1.0, jax.random.fold_in(rng, 6)
    for dim, shards_of in pieces:
        heights = jnp.exp(jax.random.uniform(jax.random.fold_in(own, dim), (shards_of,), jnp.float32, least / len(pieces), top_value / len(pieces)))
        level = level * jnp.repeat(heights, dims[dim] // shards_of).reshape([-1 if axis == dim else 1 for axis in range(len(dims))])
    return level


def scatter_about(own_key, extent, spread, reach, cuts=(), held_as=jnp.bfloat16):
    drawn = jax.random.normal(own_key, extent, jnp.float32) * spread
    if len(cuts) > 0:
        drawn = level_of(own_key, extent, cuts, -0.22, 0.18) * drawn
    return jnp.clip(drawn, min=-reach, max=reach).astype(held_as)


def setup_inputs(seed: int = 0) -> dict:
    arg_keys = jax.random.split(jax.random.key(seed), 11)
    return {
        "block_source": draw_block_source(jax.random.fold_in(arg_keys[10], 71), 0),
        "address_weights": scatter_about(arg_keys[1], (KEY_WIDTH, D), D ** -0.5, 0.125, ((0, 2),)),
        "causal_filter_taps": scatter_about(arg_keys[2], (KCONV, KEY_WIDTH), 0.5, 3.0, ((1, 2),), jnp.float32),
        "payload_vectors": scatter_about(arg_keys[3], (TOKENS, INNER), (TOKENS // 4) ** -0.5, 0.25, ((0, 16), (1, 2))),
        "probe_vectors": scatter_about(arg_keys[4], (TOKENS, KEY_WIDTH), STATE ** -0.5, 0.5, ((0, 16), (1, 2))),
        "interval_preimage": draw_interval_preimage(jax.random.fold_in(arg_keys[10], 71), 0),
        "channel_damping_exponent": draw_channel_damping_exponent(jax.random.fold_in(arg_keys[10], 71), 0),
        "added_damping_jumps": draw_added_damping_jumps(jax.random.fold_in(arg_keys[10], 71), 0),
        "sigmoid_argument": scatter_about(arg_keys[8], (TOKENS, INNER), 1.0, 6.0, ((0, 16), (1, 2))),
        "adjoint_of_result": scatter_about(arg_keys[9], (TOKENS, INNER), 1.0, 6.0, ((0, 16), (1, 2))),
    }


HIGHEST = lax.Precision.HIGHEST

def silu_slope(pre_act):
    sigma = jax.nn.sigmoid(pre_act)
    return sigma * (1.0 + pre_act * (1.0 - sigma))

def causal_conv(padded, causal_filter_taps, tokens):
    result = causal_filter_taps[0][None] * padded[0:tokens]
    for offset in range(1, causal_filter_taps.shape[0]):
        result = result + causal_filter_taps[offset][None] * padded[offset:offset + tokens]
    return result

def conv_transpose(extended, causal_filter_taps, tokens):
    tap_count = causal_filter_taps.shape[0]
    result = causal_filter_taps[0][None] * extended[tap_count - 1:tap_count - 1 + tokens]
    for offset in range(1, tap_count):
        first_row = tap_count - 1 - offset
        result = result + causal_filter_taps[offset][None] * extended[first_row:first_row + tokens]
    return result

def block_step(carry_state, inputs):
    payload_vectors, damping_exponent, key_block, probe_vectors, step_block = inputs
    block_len = payload_vectors.shape[0]
    scaled = payload_vectors * step_block[..., None]
    cumulative = jnp.cumsum(damping_exponent, axis=0)
    causal = jnp.tril(jnp.ones((block_len, block_len), dtype=bool))
    gaps = cumulative[:, None] - cumulative[None, :]
    decay_mat = jnp.exp(jnp.where(causal[:, :, None, None], gaps, -jnp.inf))
    scores = jnp.einsum('ign,jgn->gij', probe_vectors, key_block, precision=HIGHEST)
    within = jnp.einsum('gij,ijgr,jgrp->igrp', scores, decay_mat, scaled, precision=HIGHEST)
    carried = jnp.einsum('ign,grpn->igrp', probe_vectors, carry_state, precision=HIGHEST) * jnp.exp(cumulative)[..., None]
    end_decay = cumulative[-1]
    weights = jnp.exp(end_decay[None] - cumulative)
    new_state = carry_state * jnp.exp(end_decay)[..., None, None] + jnp.einsum('jgn,jgr,jgrp->grpn', key_block, weights, scaled, precision=HIGHEST)
    return (new_state, within + carried)

def linear_scan_update(payload_vectors, interval_preimage, pooled_addresses, pooled_probes, starting_memory, channel_damping_exponent, added_damping_jumps):
    tokens = pooled_addresses.shape[0]
    groups = pooled_addresses.shape[1]
    head_count = interval_preimage.shape[1]
    group_heads = head_count // groups
    block_count = tokens // BLOCK
    interval_widths = jax.nn.softplus(interval_preimage)
    damping_exponent = added_damping_jumps - jnp.exp(channel_damping_exponent)[None] * interval_widths

    def to_blocks(array):
        return array.reshape((block_count, BLOCK) + array.shape[1:])
    final_state, outputs = lax.scan(block_step, starting_memory, (to_blocks(payload_vectors.reshape(tokens, groups, group_heads, -1)), to_blocks(damping_exponent.reshape(tokens, groups, group_heads)), to_blocks(pooled_addresses), to_blocks(pooled_probes), to_blocks(interval_widths.reshape(tokens, groups, group_heads))))
    return (outputs.reshape(tokens, -1), final_state)

def reference(block_source, address_weights, causal_filter_taps, payload_vectors, probe_vectors, interval_preimage, channel_damping_exponent, added_damping_jumps, sigmoid_argument, adjoint_of_result):
    tokens = block_source.shape[0]
    channels = address_weights.shape[0]
    projected = jnp.dot(block_source, address_weights.T, preferred_element_type=jnp.float32).astype(jnp.bfloat16)
    padded = jnp.concatenate([jnp.zeros((KCONV - 1, channels), jnp.bfloat16), projected], axis=0).astype(jnp.float32)
    convolved = causal_conv(padded, causal_filter_taps, tokens)
    pooled_addresses = lax.optimization_barrier(jax.nn.silu(convolved).astype(jnp.bfloat16)).astype(jnp.float32)
    pooled_addresses = pooled_addresses.reshape(tokens, GROUPS, STATE)
    pooled_probes = probe_vectors.astype(jnp.float32).reshape(tokens, GROUPS, STATE)
    vanishing_start_memory = jnp.zeros((GROUPS, HEADS // GROUPS, HEAD_DIM, STATE), jnp.float32)

    def mixer(payload_factor, interval_argument_factor, address_factor, probe_factor):
        return linear_scan_update(payload_factor, interval_argument_factor, address_factor, probe_factor, vanishing_start_memory, channel_damping_exponent, added_damping_jumps)[0]
    mixer_out, pullback = jax.vjp(mixer, payload_vectors.astype(jnp.float32), interval_preimage, pooled_addresses, pooled_probes)
    gate_wide = sigmoid_argument.astype(jnp.float32)
    grad_wide = adjoint_of_result.astype(jnp.float32)
    mixed_grad = grad_wide * jax.nn.silu(gate_wide)
    gate_grad = (grad_wide * mixer_out * silu_slope(gate_wide)).astype(jnp.bfloat16)
    value_grad, decay_grad, key_grad, query_grad = pullback(mixed_grad)
    conv_grad = key_grad.reshape(tokens, channels) * silu_slope(convolved)
    extended = jnp.concatenate([conv_grad, jnp.zeros((KCONV - 1, channels), jnp.float32)], axis=0)
    projected_grad = conv_transpose(extended, causal_filter_taps, tokens).astype(jnp.bfloat16)
    key_weight_grad = lax.dot_general(projected_grad, block_source, (((0,), (0,)), ((), ())), preferred_element_type=jnp.float32)
    row_squares = lax.optimization_barrier(jnp.sum(key_weight_grad * key_weight_grad, axis=1))
    range_width = channels // N_TP
    input_total = jnp.zeros((block_source.shape[1], tokens), jnp.float32)
    for tp_rank in range(N_TP):
        low_edge = tp_rank * range_width
        partial_term = lax.dot_general(address_weights[low_edge:low_edge + range_width], projected_grad[:, low_edge:low_edge + range_width], (((0,), (1,)), ((), ())), preferred_element_type=jnp.float32)
        input_total = input_total + lax.optimization_barrier(partial_term.astype(jnp.bfloat16)).astype(jnp.float32)
    input_grad = input_total.astype(jnp.bfloat16)
    return (key_weight_grad, row_squares, input_grad, value_grad.astype(jnp.bfloat16), query_grad.reshape(tokens, channels).astype(jnp.bfloat16), decay_grad, gate_grad)
```

```python
import functools

import jax
import jax.numpy as jnp
from jax import lax
from jax.experimental import pallas as pl
from jax.experimental.pallas import tpu as pltpu
from jax.sharding import PartitionSpec as P

STATE = 128
F32 = jnp.float32
BF16 = jnp.bfloat16
HIGHEST = lax.Precision.HIGHEST
MESH = pl.DeviceIdType.MESH


def dot(lhs, rhs, left=1, right=0, precision=None):
    return lax.dot_general(
        lhs,
        rhs,
        (((left,), (right,)), ((), ())),
        preferred_element_type=F32,
        precision=precision,
    )


def silu_slope(pre_act):
    sigma = jax.nn.sigmoid(pre_act)
    return sigma * (1.0 + pre_act * (1.0 - sigma))


def kernel(
    cfg,
    x_ref,
    w_ref,
    taps_ref,
    val_ref,
    qry_ref,
    pre_ref,
    damp_ref,
    jump_ref,
    gate_ref,
    adj_ref,
    kwg_ref,
    rows_ref,
    ig_ref,
    vg_ref,
    qg_ref,
    dg_ref,
    gg_ref,
    xh,
    pext,
    slope,
    cta,
    u_s,
    dy_s,
    dte_s,
    ece_s,
    wee_s,
    y_s,
    du_s,
    dq_s,
    dk_s,
    s_af,
    s_ab,
    r_af,
    r_ab,
    s_bf,
    s_bb,
    r_bf,
    r_bb,
    acc_f,
    acc_b,
    wgt_f,
    wgt_b,
    s_cf,
    s_cb,
    r_cf,
    r_cb,
    ext,
    halo,
    gbuf,
    xbuf,
    rsum,
    s_r,
    r_r,
    s_i,
    r_i,
    sq,
    sem_halo,
    sem_ct,
    sem_a,
    sem_b,
    sem_c,
    sem_x,
    sem_d,
    sem_r,
    sem_i,
    sem_q,
):
    nsp, ntp, outer, inner = cfg
    i = lax.axis_index("sp")
    p = lax.axis_index("tp")
    a = i // inner
    b = i % inner
    tokens, feats = x_ref.shape
    chans = w_ref.shape[0]
    heads = pre_ref.shape[1]
    hdim = val_ref.shape[1] // heads
    groups = chans // STATE
    gcols = val_ref.shape[1] // groups
    qheads = heads // inner
    qrows = qheads * hdim
    span = feats // outer
    piece = feats // nsp
    fchunk = feats // ntp

    barrier = pltpu.get_barrier_semaphore()
    for o in range(1, nsp):
        pl.semaphore_signal(
            barrier, inc=1, device_id={"sp": (i + o) % nsp}, device_id_type=MESH
        )
    for o in range(1, ntp):
        pl.semaphore_signal(
            barrier, inc=1, device_id={"tp": (p + o) % ntp}, device_id_type=MESH
        )

    pending = []

    def send(src, dst, ssem, rsem, device, when=None):
        copy = pltpu.make_async_remote_copy(
            src_ref=src,
            dst_ref=dst,
            send_sem=ssem,
            recv_sem=rsem,
            device_id=device,
            device_id_type=MESH,
        )
        if when is None:
            copy.start()
        else:
            pl.when(when)(copy.start)
        pending.append((copy, when))

    def arrive(dst, rsem):
        pltpu.make_async_copy(dst, dst, rsem).wait()

    def at_plane(other):
        return {"sp": a * inner + other}

    def at_outer(other):
        return {"sp": other * inner + b}

    row = lax.broadcasted_iota(jnp.int32, (tokens, tokens), 0)
    col = lax.broadcasted_iota(jnp.int32, (tokens, tokens), 1)
    lower = (col <= row).astype(F32)
    upper = (row <= col).astype(F32)
    eh = lax.broadcasted_iota(jnp.int32, (heads, heads * hdim), 0)
    ec = lax.broadcasted_iota(jnp.int32, (heads, heads * hdim), 1)
    expand = (ec // hdim == eh).astype(F32)

    pre = pre_ref[...]
    rate = jnp.exp(damp_ref[...])
    step = jnp.maximum(pre, 0.0) + jnp.log1p(jnp.exp(-jnp.abs(pre)))
    decay = jump_ref[...] - rate * step
    cum = dot(lower, decay, precision=HIGHEST)
    cum_t = dot(decay, upper, 0, 0, precision=HIGHEST)
    total = dot(decay, jnp.ones((tokens, STATE), F32), 0, 0, precision=HIGHEST)
    for k in range(inner):
        cta[i, k] = total[k * qheads : (k + 1) * qheads]
    end = cum[tokens - 1 : tokens]

    pl.semaphore_wait(barrier, nsp - 1 + ntp - 1)

    send(
        x_ref.at[pl.ds(tokens - 16, 16)],
        xh,
        sem_halo.at[0],
        sem_halo.at[1],
        {"sp": (i + 1) % nsp},
        i < nsp - 1,
    )
    for o in range(1, nsp):
        peer = (i + o) % nsp
        send(cta.at[i], cta.at[i], sem_ct.at[0, o], sem_ct.at[1, i], {"sp": peer})

    ece = dot(jnp.exp(cum), expand, precision=HIGHEST)
    ece_s[...] = ece
    gate = gate_ref[...].astype(F32)
    dy = adj_ref[...].astype(F32) * (gate * jax.nn.sigmoid(gate))
    dy_s[...] = dy.astype(BF16)
    edy = (dy * ece).astype(BF16)
    for g in range(groups):
        cs = slice(g * gcols, (g + 1) * gcols)
        part = dot(edy[:, cs], qry_ref[:, g * STATE : (g + 1) * STATE], 0, 0)
        s_ab[pl.ds(g * gcols, gcols)] = part.astype(BF16)
    for o in range(1, inner):
        peer = (b + o) % inner
        send(
            s_ab.at[pl.ds(pl.multiple_of(peer * qrows, qrows), qrows)],
            r_ab.at[b],
            sem_a.at[0, 0, o],
            sem_a.at[0, 1, b],
            at_plane(peer),
        )
    r_ab[b] = s_ab[pl.ds(pl.multiple_of(b * qrows, qrows), qrows)]

    for o in range(1, outer):
        peer = (a + o) % outer
        send(
            x_ref.at[:, pl.ds(pl.multiple_of(peer * span, span), span)],
            xbuf.at[a],
            sem_x.at[0, o],
            sem_x.at[1, a],
            at_outer(peer),
        )
    xbuf[a] = x_ref[:, pl.ds(pl.multiple_of(a * span, span), span)]

    dte = dot(step, expand, precision=HIGHEST)
    dte_s[...] = dte
    wee = dot(jnp.exp(end - cum), expand, precision=HIGHEST)
    wee_s[...] = wee
    scaled = val_ref[...].astype(F32) * dte
    u_s[...] = scaled.astype(BF16)
    wu = (scaled * wee).astype(BF16)

    proj = dot(x_ref[...], w_ref[...], 1, 1)
    pext[pl.ds(16, tokens)] = proj.astype(BF16).astype(F32)

    @pl.when(i > 0)
    def _():
        arrive(xh, sem_halo.at[1])
        pext[pl.ds(0, 16)] = dot(xh[...], w_ref[...], 1, 1).astype(BF16).astype(F32)

    @pl.when(i == 0)
    def _():
        pext[pl.ds(0, 16)] = jnp.zeros((16, chans), F32)

    taps = taps_ref[...]
    ntap = taps_ref.shape[0]
    conv = taps[0:1] * pext[pl.ds(16 - (ntap - 1), tokens)]
    for k in range(1, ntap):
        conv = conv + taps[k : k + 1] * pext[pl.ds(16 - (ntap - 1) + k, tokens)]
    slope[...] = silu_slope(conv)
    keys = (conv * jax.nn.sigmoid(conv)).astype(BF16)

    for g in range(groups):
        cs = slice(g * gcols, (g + 1) * gcols)
        part = dot(wu[:, cs], keys[:, g * STATE : (g + 1) * STATE], 0, 0)
        s_af[pl.ds(g * gcols, gcols)] = part.astype(BF16)
    for o in range(1, inner):
        peer = (b + o) % inner
        send(
            s_af.at[pl.ds(pl.multiple_of(peer * qrows, qrows), qrows)],
            r_af.at[b],
            sem_a.at[1, 0, o],
            sem_a.at[1, 1, b],
            at_plane(peer),
        )
    r_af[b] = s_af[pl.ds(pl.multiple_of(b * qrows, qrows), qrows)]

    causal = col <= row

    def within(g):
        gs = slice(g * STATE, (g + 1) * STATE)
        q = qry_ref[:, gs]
        key = keys[:, gs]
        scores = dot(q, key, 1, 1)
        dscore = jnp.zeros((tokens, tokens), F32)
        for h in range(g * gcols // hdim, (g + 1) * gcols // hdim):
            hs = slice(h * hdim, (h + 1) * hdim)
            gap = cum[:, h : h + 1] - cum_t[h : h + 1, :]
            damp = jnp.exp(jnp.where(causal, gap, -jnp.inf))
            mixed = (scores * damp).astype(BF16)
            u = u_s[:, hs]
            d = dy_s[:, hs]
            dscore = dscore + dot(d, u, 1, 1) * damp
            y_s[:, hs] = dot(mixed, u)
            du_s[:, hs] = dot(mixed, d, 0, 0)
        ds = dscore.astype(BF16)
        dq_s[:, gs] = dot(ds, key)
        dk_s[:, gs] = dot(ds, q, 0, 0)

    cut1 = (groups + 1) // 2
    cut2 = cut1 + (groups - cut1 + 1) // 2
    for g in range(cut1):
        within(g)

    for o in range(1, nsp):
        src = (i + nsp - o) % nsp
        arrive(cta.at[src], sem_ct.at[1, src])

    def spread(rows):
        return jnp.concatenate(
            [jnp.broadcast_to(rows[h : h + 1], (hdim, STATE)) for h in range(qheads)], axis=0
        )

    for o in range(1, inner):
        src = (b + inner - o) % inner
        arrive(r_ab.at[src], sem_a.at[0, 1, src])
    for o in range(1, inner):
        src = (b + inner - o) % inner
        arrive(r_af.at[src], sem_a.at[1, 1, src])

    scale = [spread(jnp.exp(cta[a * inner + k, b])) for k in range(inner)]
    tot_f = r_af[0].astype(F32)
    for k in range(1, inner):
        tot_f = tot_f * scale[k] + r_af[k].astype(F32)
    tot_b = r_ab[inner - 1].astype(F32)
    for k in range(inner - 2, -1, -1):
        tot_b = tot_b * scale[k] + r_ab[k].astype(F32)
    s_bf[...] = tot_f.astype(BF16)
    s_bb[...] = tot_b.astype(BF16)
    for o in range(1, outer):
        up = (a + o) % outer
        down = (a + outer - o) % outer
        send(s_bf, r_bf.at[o], sem_b.at[0, 0, o], sem_b.at[0, 1, o], at_outer(up), a + o < outer)
        send(s_bb, r_bb.at[o], sem_b.at[1, 0, o], sem_b.at[1, 1, o], at_outer(down), a >= o)

    for g in range(cut1, cut2):
        within(g)

    acc_f[...] = jnp.zeros_like(acc_f)
    acc_b[...] = jnp.zeros_like(acc_b)
    wgt_f[...] = jnp.zeros_like(wgt_f)
    wgt_b[...] = jnp.zeros_like(wgt_b)
    for o in range(1, outer):

        @pl.when(a >= o)
        def _():
            arrive(r_bf.at[o], sem_b.at[0, 1, o])
            acc_f[...] += spread(jnp.exp(wgt_f[...])) * r_bf[o].astype(F32)
            for k in range(inner):
                wgt_f[...] += cta[(a - o) * inner + k, b]

        @pl.when(a + o < outer)
        def _():
            arrive(r_bb.at[o], sem_b.at[1, 1, o])
            acc_b[...] += spread(jnp.exp(wgt_b[...])) * r_bb[o].astype(F32)
            for k in range(inner):
                wgt_b[...] += cta[(a + o) * inner + k, b]

    run = acc_f[...]
    for k in range(inner):
        s_cf[k] = run.astype(BF16)
        if k < inner - 1:
            run = run * scale[k] + r_af[k].astype(F32)
    run = acc_b[...]
    for k in range(inner - 1, -1, -1):
        s_cb[k] = run.astype(BF16)
        if k > 0:
            run = run * scale[k] + r_ab[k].astype(F32)
    for o in range(1, inner):
        peer = (b + o) % inner
        send(s_cf.at[peer], r_cf.at[b], sem_c.at[0, 0, o], sem_c.at[0, 1, b], at_plane(peer))
        send(s_cb.at[peer], r_cb.at[b], sem_c.at[1, 0, o], sem_c.at[1, 1, b], at_plane(peer))
    r_cf[b] = s_cf[b]
    r_cb[b] = s_cb[b]

    for g in range(cut2, groups):
        within(g)

    for o in range(1, inner):
        src = (b + inner - o) % inner
        arrive(r_cf.at[src], sem_c.at[0, 1, src])
        arrive(r_cb.at[src], sem_c.at[1, 1, src])
    state = jnp.concatenate([r_cf[k] for k in range(inner)], axis=0)
    back = jnp.concatenate([r_cb[k] for k in range(inner)], axis=0)

    for g in range(groups):
        gs = slice(g * STATE, (g + 1) * STATE)
        cs = slice(g * gcols, (g + 1) * gcols)
        dk_s[:, gs] += dot(wu[:, cs], back[cs])
    cgrad = dk_s[...] * slope[...]
    ext[pl.ds(0, tokens)] = cgrad
    send(
        ext.at[pl.ds(0, 8)],
        halo,
        sem_halo.at[2],
        sem_halo.at[3],
        {"sp": (i + nsp - 1) % nsp},
        i > 0,
    )

    ones_row = jnp.ones((8, STATE), F32)
    for g in range(groups):
        gs = slice(g * STATE, (g + 1) * STATE)
        cs = slice(g * gcols, (g + 1) * gcols)
        dq_s[:, gs] += dot(edy[:, cs], state[cs])
        y_s[:, cs] += ece_s[:, cs] * dot(qry_ref[:, gs], state[cs], 1, 1)
    qg_ref[...] = dq_s[...].astype(BF16)

    @pl.when(i < nsp - 1)
    def _():
        arrive(halo, sem_halo.at[3])
        ext[pl.ds(tokens, 8)] = halo[...]

    @pl.when(i == nsp - 1)
    def _():
        ext[pl.ds(tokens, 8)] = jnp.zeros((8, chans), F32)

    pgrad = taps[0:1] * ext[pl.ds(ntap - 1, tokens)]
    for k in range(1, ntap):
        pgrad = pgrad + taps[k : k + 1] * ext[pl.ds(ntap - 1 - k, tokens)]
    pg = pgrad.astype(BF16)
    gbuf[a] = pg
    for o in range(1, outer):
        peer = (a + o) % outer
        send(gbuf.at[a], gbuf.at[a], sem_d.at[0, o], sem_d.at[1, a], at_outer(peer))

    for k in range(ntp):
        s_i[k] = dot(pg, w_ref[:, k * fchunk : (k + 1) * fchunk]).astype(BF16)
    for o in range(1, ntp):
        peer = (p + o) % ntp
        send(s_i.at[peer], r_i.at[p], sem_i.at[0, o], sem_i.at[1, p], {"tp": peer})
    r_i[p] = s_i[p]

    inter = []
    for g in range(groups):
        gs = slice(g * STATE, (g + 1) * STATE)
        cs = slice(g * gcols, (g + 1) * gcols)
        kg = wee_s[:, cs] * dot(keys[:, gs], back[cs], 1, 1)
        du_s[:, cs] += kg
        carry = dot(jnp.ones((8, tokens), F32), u_s[:, cs].astype(F32) * kg, precision=HIGHEST)
        both = state[cs].astype(F32) * back[cs].astype(F32)
        carry = carry + ece_s[tokens - 1 : tokens, cs] * dot(
            ones_row, both, 1, 1, precision=HIGHEST
        )
        inter.append(carry)
    inter = dot(jnp.concatenate(inter, axis=1), expand, 1, 1, precision=HIGHEST)[0:1]
    vg_ref[...] = (du_s[...] * dte_s[...]).astype(BF16)
    adj = adj_ref[...].astype(F32)
    gate2 = gate_ref[...].astype(F32)
    gg_ref[...] = (adj * y_s[...] * silu_slope(gate2)).astype(BF16)
    moved = dy_s[...].astype(F32) * y_s[...] - u_s[...].astype(F32) * du_s[...]
    dcum = dot(moved, expand, 1, 1, precision=HIGHEST)
    ddecay = dot(upper, dcum, precision=HIGHEST) + inter
    dstep = dot(val_ref[...].astype(F32) * du_s[...], expand, 1, 1, precision=HIGHEST)
    dg_ref[...] = (dstep - rate * ddecay) * jax.nn.sigmoid(pre)

    for o in range(1, outer):
        src = (a + outer - o) % outer
        arrive(xbuf.at[src], sem_x.at[1, src])
    grads = dot(gbuf[a], xbuf[a], 0, 0)
    for o in range(1, outer):
        src = (a + outer - o) % outer
        arrive(gbuf.at[src], sem_d.at[1, src])
        grads = grads + dot(gbuf[src], xbuf[src], 0, 0)
    for k in range(inner):
        part = grads[:, k * piece : (k + 1) * piece]
        rsum[k] = part
        s_r[k] = part.astype(BF16)
    for o in range(1, inner):
        peer = (b + o) % inner
        send(s_r.at[peer], r_r.at[b], sem_r.at[0, o], sem_r.at[1, b], at_plane(peer))

    for o in range(1, ntp):
        src = (p + ntp - o) % ntp
        arrive(r_i.at[src], sem_i.at[1, src])
    summed = r_i[0].astype(F32)
    for k in range(1, ntp):
        summed = summed + r_i[k].astype(F32)
    ig_ref[...] = summed.T.astype(BF16)

    kwg = rsum[b]
    for o in range(1, inner):
        src = (b + inner - o) % inner
        arrive(r_r.at[src], sem_r.at[1, src])
        kwg = kwg + r_r[src].astype(F32)
    squares = dot(jnp.ones((8, piece), F32), kwg * kwg, 1, 1, precision=HIGHEST)
    sq[i] = squares[0:1]
    for o in range(1, nsp):
        peer = (i + o) % nsp
        send(sq.at[i], sq.at[i], sem_q.at[0, o], sem_q.at[1, i], {"sp": peer})
    kwg_ref[...] = kwg
    for o in range(1, nsp):
        src = (i + nsp - o) % nsp
        arrive(sq.at[src], sem_q.at[1, src])
    result = sq[0]
    for k in range(1, nsp):
        result = result + sq[k]
    rows_ref[...] = result

    for copy, when in pending:
        if when is None:
            copy.wait_send()
        else:
            pl.when(when)(copy.wait_send)


def per_device(cfg, *args):
    x, w, taps, val, qry, pre, damp, jump, gate, adj = args
    nsp, ntp, outer, inner = cfg
    tokens, feats = x.shape
    chans = w.shape[0]
    heads = pre.shape[1]
    width = val.shape[1]
    qheads = heads // inner
    qrows = width // inner
    piece = feats // nsp
    fchunk = feats // ntp
    dma = pltpu.SemaphoreType.DMA
    V = pltpu.VMEM
    scratch = [
        V((16, feats), BF16),
        V((tokens + 16, chans), F32),
        V((tokens, chans), F32),
        V((nsp, inner, qheads, STATE), F32),
        V((tokens, width), BF16),
        V((tokens, width), BF16),
        V((tokens, width), F32),
        V((tokens, width), F32),
        V((tokens, width), F32),
        V((tokens, width), F32),
        V((tokens, width), F32),
        V((tokens, chans), F32),
        V((tokens, chans), F32),
        V((width, STATE), BF16),
        V((width, STATE), BF16),
        V((inner, qrows, STATE), BF16),
        V((inner, qrows, STATE), BF16),
        V((qrows, STATE), BF16),
        V((qrows, STATE), BF16),
        V((outer, qrows, STATE), BF16),
        V((outer, qrows, STATE), BF16),
        V((qrows, STATE), F32),
        V((qrows, STATE), F32),
        V((qheads, STATE), F32),
        V((qheads, STATE), F32),
        V((inner, qrows, STATE), BF16),
        V((inner, qrows, STATE), BF16),
        V((inner, qrows, STATE), BF16),
        V((inner, qrows, STATE), BF16),
        V((tokens + 8, chans), F32),
        V((8, chans), F32),
        V((outer, tokens, chans), BF16),
        V((outer, tokens, feats // outer), BF16),
        V((inner, chans, piece), F32),
        V((inner, chans, piece), BF16),
        V((inner, chans, piece), BF16),
        V((ntp, tokens, fchunk), BF16),
        V((ntp, tokens, fchunk), BF16),
        V((nsp, 1, chans), F32),
        dma((4,)),
        dma((2, nsp)),
        dma((2, 2, inner)),
        dma((2, 2, outer)),
        dma((2, 2, inner)),
        dma((2, outer)),
        dma((2, outer)),
        dma((2, inner)),
        dma((2, ntp)),
        dma((2, nsp)),
    ]
    out_shape = (
        jax.ShapeDtypeStruct((chans, piece), F32),
        jax.ShapeDtypeStruct((1, chans), F32),
        jax.ShapeDtypeStruct((fchunk, tokens), BF16),
        jax.ShapeDtypeStruct((tokens, width), BF16),
        jax.ShapeDtypeStruct((tokens, chans), BF16),
        jax.ShapeDtypeStruct((tokens, heads), F32),
        jax.ShapeDtypeStruct((tokens, width), BF16),
    )
    vmem = pl.BlockSpec(memory_space=pltpu.VMEM)
    outs = pl.pallas_call(
        functools.partial(kernel, cfg),
        out_shape=out_shape,
        in_specs=[vmem] * 10,
        out_specs=(vmem,) * 7,
        scratch_shapes=scratch,
        compiler_params=pltpu.CompilerParams(
            collective_id=0, has_side_effects=True, vmem_limit_bytes=56 * 2**20
        ),
    )(x, w, taps, val, qry, pre, damp.reshape(1, heads), jump, gate, adj)
    return (outs[0], outs[1].reshape(chans)) + tuple(outs[2:])


def solution(mesh):
    nsp, ntp = mesh.shape["sp"], mesh.shape["tp"]
    inner = 4
    cfg = (nsp, ntp, nsp // inner, inner)
    tokens = P("sp", "tp")
    in_specs = (
        P("sp", None),
        P("tp", None),
        P(None, "tp"),
        tokens,
        tokens,
        tokens,
        P("tp"),
        tokens,
        tokens,
        tokens,
    )
    out_specs = (P("tp", "sp"), P("tp"), P("tp", "sp"), tokens, tokens, tokens, tokens)
    return jax.shard_map(
        functools.partial(per_device, cfg),
        mesh=mesh,
        in_specs=in_specs,
        out_specs=out_specs,
        check_vma=False,
    )
```

```python
import functools

import jax
import jax.numpy as jnp
from jax import lax
from jax.experimental import pallas as pl
from jax.experimental.pallas import tpu as pltpu
from jax.sharding import PartitionSpec as P

STATE = 128
F32 = jnp.float32
BF16 = jnp.bfloat16
HIGHEST = lax.Precision.HIGHEST
MESH = pl.DeviceIdType.MESH


def dot(lhs, rhs, left=1, right=0, precision=None):
    return lax.dot_general(
        lhs,
        rhs,
        (((left,), (right,)), ((), ())),
        preferred_element_type=F32,
        precision=precision,
    )


def silu_slope(pre_act):
    sigma = jax.nn.sigmoid(pre_act)
    return sigma * (1.0 + pre_act * (1.0 - sigma))


def kernel(
    cfg,
    x_hbm,
    w_hbm,
    taps_ref,
    val_ref,
    qry_ref,
    pre_ref,
    damp_ref,
    jump_ref,
    gate_ref,
    adj_ref,
    kwg_ref,
    rows_ref,
    ig_ref,
    vg_ref,
    qg_ref,
    dg_ref,
    gg_ref,
    x_ref,
    w_ref,
    xh,
    pext,
    slope,
    cta,
    u_s,
    dy_s,
    dte_s,
    ece_s,
    wee_s,
    y_s,
    du_s,
    dq_s,
    dk_s,
    s_af,
    s_ab,
    r_af,
    r_ab,
    s_bf,
    s_bb,
    r_bf,
    r_bb,
    acc_f,
    acc_b,
    wgt_f,
    wgt_b,
    s_cf,
    s_cb,
    r_cf,
    r_cb,
    ext,
    halo,
    gbuf,
    xbuf,
    rsum,
    s_r,
    r_r,
    s_i,
    r_i,
    sq,
    sem_halo,
    sem_ct,
    sem_a,
    sem_b,
    sem_c,
    sem_x,
    sem_d,
    sem_r,
    sem_i,
    sem_q,
    sem_y,
    sem_l,
):
    nsp, ntp, outer, inner = cfg
    i = lax.axis_index("sp")
    p = lax.axis_index("tp")
    a = i // inner
    b = i % inner
    tokens, feats = x_ref.shape
    chans = w_ref.shape[0]
    heads = pre_ref.shape[0]
    hdim = val_ref.shape[1] // heads
    groups = chans // STATE
    gcols = val_ref.shape[1] // groups
    qheads = heads // inner
    qrows = qheads * hdim
    span = feats // outer
    piece = feats // nsp
    fchunk = feats // ntp
    share = tokens // ntp
    halves = gbuf.shape[0]
    hchan = chans // halves

    load_x = pltpu.make_async_copy(x_hbm, x_ref, sem_l.at[0])
    load_w = pltpu.make_async_copy(w_hbm, w_ref, sem_l.at[1])
    load_x.start()
    load_w.start()
    barrier = pltpu.get_barrier_semaphore()
    for o in range(1, nsp):
        pl.semaphore_signal(
            barrier, inc=1, device_id={"sp": (i + o) % nsp}, device_id_type=MESH
        )
    for o in range(1, ntp):
        pl.semaphore_signal(
            barrier, inc=1, device_id={"tp": (p + o) % ntp}, device_id_type=MESH
        )

    pending = []

    def send(src, dst, ssem, rsem, device, when=None):
        copy = pltpu.make_async_remote_copy(
            src_ref=src,
            dst_ref=dst,
            send_sem=ssem,
            recv_sem=rsem,
            device_id=device,
            device_id_type=MESH,
        )
        if when is None:
            copy.start()
        else:
            pl.when(when)(copy.start)
        pending.append((copy, when))

    def arrive(dst, rsem):
        pltpu.make_async_copy(dst, dst, rsem).wait()

    def at_plane(other):
        return {"sp": a * inner + other}

    def at_outer(other):
        return {"sp": other * inner + b}

    row = lax.broadcasted_iota(jnp.int32, (tokens, tokens), 0)
    col = lax.broadcasted_iota(jnp.int32, (tokens, tokens), 1)
    lower = (col <= row).astype(F32)
    upper = (row <= col).astype(F32)
    eh = lax.broadcasted_iota(jnp.int32, (heads, heads * hdim), 0)
    ec = lax.broadcasted_iota(jnp.int32, (heads, heads * hdim), 1)
    expand = (ec // hdim == eh).astype(F32)

    pre = pre_ref[...].T
    rate = jnp.exp(damp_ref[...])
    step = jnp.maximum(pre, 0.0) + jnp.log1p(jnp.exp(-jnp.abs(pre)))
    decay = jump_ref[...].T - rate * step
    cum = dot(lower, decay, precision=HIGHEST)
    cum_t = dot(decay, upper, 0, 0, precision=HIGHEST)
    total = dot(decay, jnp.ones((tokens, STATE), F32), 0, 0, precision=HIGHEST)
    for k in range(inner):
        cta[i, k] = total[k * qheads : (k + 1) * qheads]
    end = cum[tokens - 1 : tokens]

    ece = dot(jnp.exp(cum), expand, precision=HIGHEST)
    ece_s[...] = ece
    gate = gate_ref[...].astype(F32)
    dy = adj_ref[...].astype(F32) * (gate * jax.nn.sigmoid(gate))
    dy_s[...] = dy.astype(BF16)
    edy = (dy * ece).astype(BF16)
    for g in range(groups):
        cs = slice(g * gcols, (g + 1) * gcols)
        part = dot(edy[:, cs], qry_ref[:, g * STATE : (g + 1) * STATE], 0, 0)
        s_ab[pl.ds(g * gcols, gcols)] = part.astype(BF16)
    load_x.wait()

    pl.semaphore_wait(barrier, nsp - 1 + ntp - 1)

    for o in range(1, inner):
        peer = (b + o) % inner
        other = a * inner + peer
        send(cta.at[i], cta.at[i], sem_ct.at[0, other], sem_ct.at[1, i], {"sp": other})
        send(
            s_ab.at[pl.ds(pl.multiple_of(peer * qrows, qrows), qrows)],
            r_ab.at[b],
            sem_a.at[0, 0, o],
            sem_a.at[0, 1, b],
            at_plane(peer),
        )
    send(
        x_ref.at[pl.ds(tokens - 16, 16)],
        xh,
        sem_halo.at[0],
        sem_halo.at[1],
        {"sp": (i + 1) % nsp},
        i < nsp - 1,
    )
    for o in range(1, outer):
        for k in range(inner):
            other = (a + o) % outer * inner + k
            send(cta.at[i], cta.at[i], sem_ct.at[0, other], sem_ct.at[1, i], {"sp": other})
    r_ab[b] = s_ab[pl.ds(pl.multiple_of(b * qrows, qrows), qrows)]

    mine = pl.ds(pl.multiple_of(p * share, share), share)
    for o in range(1, outer):
        peer = (a + o) % outer
        send(
            x_ref.at[mine, pl.ds(pl.multiple_of(peer * span, span), span)],
            xbuf.at[a, mine],
            sem_x.at[0, o],
            sem_x.at[1, a],
            at_outer(peer),
        )
    xbuf[a] = x_ref[:, pl.ds(pl.multiple_of(a * span, span), span)]

    dte = dot(step, expand, precision=HIGHEST)
    dte_s[...] = dte
    wee = dot(jnp.exp(end - cum), expand, precision=HIGHEST)
    wee_s[...] = wee
    scaled = val_ref[...].astype(F32) * dte
    u_s[...] = scaled.astype(BF16)
    wu = (scaled * wee).astype(BF16)

    load_w.wait()
    proj = dot(x_ref[...], w_ref[...], 1, 1)
    pext[pl.ds(16, tokens)] = proj.astype(BF16).astype(F32)

    @pl.when(i > 0)
    def _():
        arrive(xh, sem_halo.at[1])
        pext[pl.ds(0, 16)] = dot(xh[...], w_ref[...], 1, 1).astype(BF16).astype(F32)

    @pl.when(i == 0)
    def _():
        pext[pl.ds(0, 16)] = jnp.zeros((16, chans), F32)

    taps = taps_ref[...]
    ntap = taps_ref.shape[0]
    conv = taps[0:1] * pext[pl.ds(16 - (ntap - 1), tokens)]
    for k in range(1, ntap):
        conv = conv + taps[k : k + 1] * pext[pl.ds(16 - (ntap - 1) + k, tokens)]
    slope[...] = silu_slope(conv)
    keys = (conv * jax.nn.sigmoid(conv)).astype(BF16)

    for g in range(groups):
        cs = slice(g * gcols, (g + 1) * gcols)
        part = dot(wu[:, cs], keys[:, g * STATE : (g + 1) * STATE], 0, 0)
        s_af[pl.ds(g * gcols, gcols)] = part.astype(BF16)
    for o in range(1, inner):
        peer = (b + o) % inner
        send(
            s_af.at[pl.ds(pl.multiple_of(peer * qrows, qrows), qrows)],
            r_af.at[b],
            sem_a.at[1, 0, o],
            sem_a.at[1, 1, b],
            at_plane(peer),
        )
    r_af[b] = s_af[pl.ds(pl.multiple_of(b * qrows, qrows), qrows)]

    causal = col <= row

    def within(g):
        gs = slice(g * STATE, (g + 1) * STATE)
        q = qry_ref[:, gs]
        key = keys[:, gs]
        scores = dot(q, key, 1, 1)
        dscore = jnp.zeros((tokens, tokens), F32)
        for h in range(g * gcols // hdim, (g + 1) * gcols // hdim):
            hs = slice(h * hdim, (h + 1) * hdim)
            gap = cum[:, h : h + 1] - cum_t[h : h + 1, :]
            damp = jnp.exp(jnp.where(causal, gap, -jnp.inf))
            mixed = (scores * damp).astype(BF16)
            u = u_s[:, hs]
            d = dy_s[:, hs]
            dscore = dscore + dot(d, u, 1, 1) * damp
            y_s[:, hs] = dot(mixed, u)
            du_s[:, hs] = dot(mixed, d, 0, 0)
        ds = dscore.astype(BF16)
        dq_s[:, gs] = dot(ds, key)
        dk_s[:, gs] = dot(ds, q, 0, 0)

    def spread(rows):
        return jnp.concatenate(
            [jnp.broadcast_to(rows[h : h + 1], (hdim, STATE)) for h in range(qheads)], axis=0
        )

    for o in range(1, inner):
        src = (b + inner - o) % inner
        arrive(cta.at[a * inner + src], sem_ct.at[1, a * inner + src])
        arrive(r_ab.at[src], sem_a.at[0, 1, src])
    scale = [spread(jnp.exp(cta[a * inner + k, b])) for k in range(inner)]
    tot_b = r_ab[inner - 1].astype(F32)
    for k in range(inner - 2, -1, -1):
        tot_b = tot_b * scale[k] + r_ab[k].astype(F32)
    s_bb[...] = tot_b.astype(BF16)
    for o in range(1, outer):
        down = (a + outer - o) % outer
        send(s_bb, r_bb.at[o], sem_b.at[1, 0, o], sem_b.at[1, 1, o], at_outer(down), a >= o)

    cut = (groups + 1) // 2
    within(0)

    for o in range(1, inner):
        src = (b + inner - o) % inner
        arrive(r_af.at[src], sem_a.at[1, 1, src])
    tot_f = r_af[0].astype(F32)
    for k in range(1, inner):
        tot_f = tot_f * scale[k] + r_af[k].astype(F32)
    s_bf[...] = tot_f.astype(BF16)
    for o in range(1, outer):
        up = (a + o) % outer
        send(s_bf, r_bf.at[o], sem_b.at[0, 0, o], sem_b.at[0, 1, o], at_outer(up), a + o < outer)

    for o in range(1, outer):
        src = (a + outer - o) % outer
        arrive(xbuf.at[src, mine], sem_x.at[1, src])
        for t in range(1, ntp):
            send(
                xbuf.at[src, mine],
                xbuf.at[src, mine],
                sem_y.at[0, o, t],
                sem_y.at[1, src, p],
                {"tp": (p + t) % ntp},
            )

    for g in range(1, cut):
        within(g)
    for o in range(1, outer):
        for k in range(inner):
            src = (a + outer - o) % outer * inner + k
            arrive(cta.at[src], sem_ct.at[1, src])

    acc_b[...] = jnp.zeros_like(acc_b)
    wgt_b[...] = jnp.zeros_like(wgt_b)
    for o in range(1, outer):

        @pl.when(a + o < outer)
        def _():
            arrive(r_bb.at[o], sem_b.at[1, 1, o])
            acc_b[...] += spread(jnp.exp(wgt_b[...])) * r_bb[o].astype(F32)
            for k in range(inner):
                wgt_b[...] += cta[(a + o) * inner + k, b]

    run = acc_b[...]
    for k in range(inner - 1, -1, -1):
        s_cb[k] = run.astype(BF16)
        if k > 0:
            run = run * scale[k] + r_ab[k].astype(F32)
    for o in range(1, inner):
        peer = (b + o) % inner
        send(s_cb.at[peer], r_cb.at[b], sem_c.at[1, 0, o], sem_c.at[1, 1, b], at_plane(peer))
    r_cb[b] = s_cb[b]

    for g in range(cut, groups):
        within(g)

    acc_f[...] = jnp.zeros_like(acc_f)
    wgt_f[...] = jnp.zeros_like(wgt_f)
    for o in range(1, outer):

        @pl.when(a >= o)
        def _():
            arrive(r_bf.at[o], sem_b.at[0, 1, o])
            acc_f[...] += spread(jnp.exp(wgt_f[...])) * r_bf[o].astype(F32)
            for k in range(inner):
                wgt_f[...] += cta[(a - o) * inner + k, b]

    run = acc_f[...]
    for k in range(inner):
        s_cf[k] = run.astype(BF16)
        if k < inner - 1:
            run = run * scale[k] + r_af[k].astype(F32)
    for o in range(1, inner):
        peer = (b + o) % inner
        send(s_cf.at[peer], r_cf.at[b], sem_c.at[0, 0, o], sem_c.at[0, 1, b], at_plane(peer))
    r_cf[b] = s_cf[b]

    for o in range(1, inner):
        src = (b + inner - o) % inner
        arrive(r_cb.at[src], sem_c.at[1, 1, src])
    back = jnp.concatenate([r_cb[k] for k in range(inner)], axis=0)

    for g in range(groups):
        gs = slice(g * STATE, (g + 1) * STATE)
        cs = slice(g * gcols, (g + 1) * gcols)
        dk_s[:, gs] += dot(wu[:, cs], back[cs])
    cgrad = dk_s[...] * slope[...]
    ext[pl.ds(0, tokens)] = cgrad
    send(
        ext.at[pl.ds(0, 8)],
        halo,
        sem_halo.at[2],
        sem_halo.at[3],
        {"sp": (i + nsp - 1) % nsp},
        i > 0,
    )

    def backs(g):
        gs = slice(g * STATE, (g + 1) * STATE)
        cs = slice(g * gcols, (g + 1) * gcols)
        return wee_s[:, cs] * dot(keys[:, gs], back[cs], 1, 1)

    pulled = [backs(g) for g in range(groups)]
    for g in range(groups):
        cs = slice(g * gcols, (g + 1) * gcols)
        du_s[:, cs] += pulled[g]
    vg_ref[...] = (du_s[...] * dte_s[...]).astype(BF16)

    @pl.when(i < nsp - 1)
    def _():
        arrive(halo, sem_halo.at[3])
        ext[pl.ds(tokens, 8)] = halo[...]

    @pl.when(i == nsp - 1)
    def _():
        ext[pl.ds(tokens, 8)] = jnp.zeros((8, chans), F32)

    pgrad = taps[0:1] * ext[pl.ds(ntap - 1, tokens)]
    for k in range(1, ntap):
        pgrad = pgrad + taps[k : k + 1] * ext[pl.ds(ntap - 1 - k, tokens)]
    pg = pgrad.astype(BF16)
    for f in range(halves):
        gbuf[f, a] = pg[:, f * hchan : (f + 1) * hchan]
    for f in range(halves):
        for o in range(1, outer):
            peer = (a + o) % outer
            send(
                gbuf.at[f, a],
                gbuf.at[f, a],
                sem_d.at[0, f, o],
                sem_d.at[1, f, a],
                at_outer(peer),
            )

    for k in range(ntp):
        s_i[k] = dot(pg, w_ref[:, k * fchunk : (k + 1) * fchunk]).astype(BF16)
    for o in range(1, ntp):
        peer = (p + o) % ntp
        send(s_i.at[peer], r_i.at[p], sem_i.at[0, o], sem_i.at[1, p], {"tp": peer})
    r_i[p] = s_i[p]

    for o in range(1, inner):
        src = (b + inner - o) % inner
        arrive(r_cf.at[src], sem_c.at[0, 1, src])
    state = jnp.concatenate([r_cf[k] for k in range(inner)], axis=0)
    for g in range(groups):
        gs = slice(g * STATE, (g + 1) * STATE)
        cs = slice(g * gcols, (g + 1) * gcols)
        dq_s[:, gs] += dot(edy[:, cs], state[cs])
        y_s[:, cs] += ece_s[:, cs] * dot(qry_ref[:, gs], state[cs], 1, 1)
    qg_ref[...] = dq_s[...].astype(BF16)

    for o in range(1, outer):
        src = (a + outer - o) % outer
        for t in range(1, ntp):
            q = (p + ntp - t) % ntp
            rows = pl.ds(pl.multiple_of(q * share, share), share)
            arrive(xbuf.at[src, rows], sem_y.at[1, src, q])
    for f in range(halves):
        grads = dot(gbuf[f, a], xbuf[a], 0, 0)
        for o in range(1, outer):
            src = (a + outer - o) % outer
            arrive(gbuf.at[f, src], sem_d.at[1, f, src])
            grads = grads + dot(gbuf[f, src], xbuf[src], 0, 0)
        for k in range(inner):
            part = grads[:, k * piece : (k + 1) * piece]
            rsum[f, k] = part
            s_r[f, k] = part.astype(BF16)
        for o in range(1, inner):
            peer = (b + o) % inner
            send(
                s_r.at[f, peer],
                r_r.at[f, b],
                sem_r.at[0, f, o],
                sem_r.at[1, f, b],
                at_plane(peer),
            )

    for o in range(1, ntp):
        src = (p + ntp - o) % ntp
        arrive(r_i.at[src], sem_i.at[1, src])
    summed = r_i[0].astype(F32)
    for k in range(1, ntp):
        summed = summed + r_i[k].astype(F32)
    ig_ref[...] = summed.T.astype(BF16)

    gg_ref[...] = (
        adj_ref[...].astype(F32) * y_s[...] * silu_slope(gate_ref[...].astype(F32))
    ).astype(BF16)

    for f in range(halves):
        kwg = rsum[f, b]
        for o in range(1, inner):
            src = (b + inner - o) % inner
            arrive(r_r.at[f, src], sem_r.at[1, f, src])
            kwg = kwg + r_r[f, src].astype(F32)
        squares = dot(jnp.ones((8, piece), F32), kwg * kwg, 1, 1, precision=HIGHEST)
        sq[i, :, f * hchan : (f + 1) * hchan] = squares[0:1]
        kwg_ref[f * hchan : (f + 1) * hchan] = kwg
    for o in range(1, nsp):
        peer = (i + o) % nsp
        send(sq.at[i], sq.at[i], sem_q.at[0, o], sem_q.at[1, i], {"sp": peer})

    inter = []
    for g in range(groups):
        cs = slice(g * gcols, (g + 1) * gcols)
        carry = dot(
            jnp.ones((8, tokens), F32), u_s[:, cs].astype(F32) * pulled[g], precision=HIGHEST
        )
        both = state[cs].astype(F32) * back[cs].astype(F32)
        carry = carry + ece_s[tokens - 1 : tokens, cs] * dot(
            jnp.ones((8, STATE), F32), both, 1, 1, precision=HIGHEST
        )
        inter.append(carry)
    inter = dot(jnp.concatenate(inter, axis=1), expand, 1, 1, precision=HIGHEST)[0:1]
    moved = dy_s[...].astype(F32) * y_s[...] - u_s[...].astype(F32) * du_s[...]
    dcum = dot(moved, expand, 1, 1, precision=HIGHEST)
    ddecay = dot(upper, dcum, precision=HIGHEST) + inter
    dstep = dot(val_ref[...].astype(F32) * du_s[...], expand, 1, 1, precision=HIGHEST)
    dg_ref[...] = ((dstep - rate * ddecay) * jax.nn.sigmoid(pre)).T

    for o in range(1, nsp):
        src = (i + nsp - o) % nsp
        arrive(sq.at[src], sem_q.at[1, src])
    result = sq[0]
    for k in range(1, nsp):
        result = result + sq[k]
    rows_ref[...] = result

    for copy, when in pending:
        if when is None:
            copy.wait_send()
        else:
            pl.when(when)(copy.wait_send)


def finish(*refs):
    count = len(refs) // 2
    for src, dst in zip(refs[:count], refs[count:]):
        dst[...] = src[...]


def per_device(cfg, *args):
    x, w, taps, val, qry, pre, damp, jump, gate, adj = args
    nsp, ntp, outer, inner = cfg
    tokens, feats = x.shape
    chans = w.shape[0]
    heads = pre.shape[1]
    halves = 2 if chans > STATE else 1
    width = val.shape[1]
    qheads = heads // inner
    qrows = width // inner
    piece = feats // nsp
    fchunk = feats // ntp
    dma = pltpu.SemaphoreType.DMA
    V = pltpu.VMEM
    scratch = [
        V((tokens, feats), BF16),
        V((chans, feats), BF16),
        V((16, feats), BF16),
        V((tokens + 16, chans), F32),
        V((tokens, chans), F32),
        V((nsp, inner, qheads, STATE), F32),
        V((tokens, width), BF16),
        V((tokens, width), BF16),
        V((tokens, width), F32),
        V((tokens, width), F32),
        V((tokens, width), F32),
        V((tokens, width), F32),
        V((tokens, width), F32),
        V((tokens, chans), F32),
        V((tokens, chans), F32),
        V((width, STATE), BF16),
        V((width, STATE), BF16),
        V((inner, qrows, STATE), BF16),
        V((inner, qrows, STATE), BF16),
        V((qrows, STATE), BF16),
        V((qrows, STATE), BF16),
        V((outer, qrows, STATE), BF16),
        V((outer, qrows, STATE), BF16),
        V((qrows, STATE), F32),
        V((qrows, STATE), F32),
        V((qheads, STATE), F32),
        V((qheads, STATE), F32),
        V((inner, qrows, STATE), BF16),
        V((inner, qrows, STATE), BF16),
        V((inner, qrows, STATE), BF16),
        V((inner, qrows, STATE), BF16),
        V((tokens + 8, chans), F32),
        V((8, chans), F32),
        V((halves, outer, tokens, chans // halves), BF16),
        V((outer, tokens, feats // outer), BF16),
        V((halves, inner, chans // halves, piece), F32),
        V((halves, inner, chans // halves, piece), BF16),
        V((halves, inner, chans // halves, piece), BF16),
        V((ntp, tokens, fchunk), BF16),
        V((ntp, tokens, fchunk), BF16),
        V((nsp, 1, chans), F32),
        dma((4,)),
        dma((2, nsp)),
        dma((2, 2, inner)),
        dma((2, 2, outer)),
        dma((2, 2, inner)),
        dma((2, outer)),
        dma((2, halves, outer)),
        dma((2, halves, inner)),
        dma((2, ntp)),
        dma((2, nsp)),
        dma((2, outer, ntp)),
        dma((2,)),
    ]
    out_shape = (
        jax.ShapeDtypeStruct((chans, piece), F32),
        jax.ShapeDtypeStruct((1, chans), F32),
        jax.ShapeDtypeStruct((fchunk, tokens), BF16),
        jax.ShapeDtypeStruct((tokens, width), BF16),
        jax.ShapeDtypeStruct((tokens, chans), BF16),
        jax.ShapeDtypeStruct((heads, tokens), F32),
        jax.ShapeDtypeStruct((tokens, width), BF16),
    )
    vmem = pl.BlockSpec(memory_space=pltpu.VMEM)
    outs = pl.pallas_call(
        functools.partial(kernel, cfg),
        out_shape=out_shape,
        in_specs=[pl.BlockSpec(memory_space=pl.ANY)] * 2 + [vmem] * 8,
        out_specs=(vmem,) * 7,
        scratch_shapes=scratch,
        compiler_params=pltpu.CompilerParams(
            collective_id=0, has_side_effects=True, vmem_limit_bytes=24 * 2**20
        ),
    )(x, w, taps, val, qry, pre.T, damp.reshape(1, heads), jump.T, gate, adj)
    outs = pl.pallas_call(
        finish,
        out_shape=out_shape,
        in_specs=[vmem] * 7,
        out_specs=(vmem,) * 7,
        compiler_params=pltpu.CompilerParams(vmem_limit_bytes=16 * 2**20),
    )(*outs)
    return (outs[0], outs[1].reshape(chans)) + tuple(outs[2:5]) + (outs[5].T, outs[6])


def solution(mesh):
    nsp, ntp = mesh.shape["sp"], mesh.shape["tp"]
    inner = 4
    cfg = (nsp, ntp, nsp // inner, inner)
    tokens = P("sp", "tp")
    in_specs = (
        P("sp", None),
        P("tp", None),
        P(None, "tp"),
        tokens,
        tokens,
        tokens,
        P("tp"),
        tokens,
        tokens,
        tokens,
    )
    out_specs = (P("tp", "sp"), P("tp"), P("tp", "sp"), tokens, tokens, tokens, tokens)
    return jax.shard_map(
        functools.partial(per_device, cfg),
        mesh=mesh,
        in_specs=in_specs,
        out_specs=out_specs,
        check_vma=False,
    )
```
